256 devices in a mesh: ep: 64 (over z, y, core), tp: 4 (over x).
Axes of the slice: x: 4, y: 4, z: 8, core: 2. Of those that a mesh axis runs over, the one named last changes fastest.
Arguments:
- cell_query_rows: bfloat16 [16384, 2048], P('ep', 'tp'), may hold values from -6 to 6
- cell_key_rows: bfloat16 [16384, 2048], P('ep', 'tp'), may hold values from -6 to 6
- cell_value_rows: bfloat16 [16384, 2048], P('ep', 'tp'), may hold values from -6 to 6
- output_gate_logits: bfloat16 [16384, 2048], P('ep', 'tp'), may hold values from -8 to 8
- log_input_gate: float32 [8, 16384], P('tp', 'ep'), may hold values from -4 to 110
- forget_gate_logits: float32 [8, 16384], P('tp', 'ep'), may hold values from -1 to 25
- extra_log_forget: float32 [8, 16384], P('tp', 'ep'), may hold values from -0.7 to 0
- cell_output_scale: float32 [2048], P('tp'), may hold values from 0.1 to 1.9
- tokens_into_experts: bfloat16 [32768, 2048], P(('ep', 'tp')), may hold values from -6 to 6
- expert_norm_scale: float32 [2048], replicated, may hold values from 0.1 to 1.9
- token_expert_index: int32 [32768, 2], P(('ep', 'tp')), may hold values from 0 to 63, all different within a row; in each aligned block of 128 rows (0 to 127, 128 to 255, ...) at most 5 rows name the same one
- chosen_expert_weight: float32 [32768, 2], P(('ep', 'tp')), may hold values from 0.3 to 3
- expert_gate_weight: bfloat16 [64, 2048, 3584], P('ep', None, 'tp'), may hold values from -0.125 to 0.125
- expert_up_weight: bfloat16 [64, 2048, 3584], P('ep', None, 'tp'), may hold values from -0.125 to 0.125
- expert_down_weight: bfloat16 [64, 3584, 2048], P('ep', 'tp'), may hold values from -0.09375 to 0.09375
Outputs:
- gated_head_output: bfloat16 [16384, 2048], P('ep', 'tp')
- expert_output: bfloat16 [32768, 2048], P(('ep', 'tp'))
The draws below stay inside these ranges and needn't reach their ends.
Inputs may be any that keep to these rules, and one draw needn't show every extreme that they name: `token_expert_index`: each row names 2 different experts. Among the rows of one device (aligned blocks of 128 rows) no expert is named by more than 5 rows, and in every draw some expert is named by exactly 5 rows of some device.
All inputs are finite; a program needn't handle non-finite values.
Results may differ from the reference program's by a relative error of at most 0.012.
Values may be sent and summed in bfloat16 or wider, within the bound.
No kernel may reach another device: no remote copies, remote signals or barrier semaphores. Data moves between devices by JAX's collectives and lax.ppermute only.
A program may use at most 128 MiB of HBM per device.

```python
import math
import jax
import jax.numpy as jnp
import numpy as np
from jax import lax

D = 2048
HEAD_DIM = 256
HEADS = 8
BLOCK = 64
FF = 3584
TOPK = 2
MIX_DEV = 256
MOE_DEV = 128
INNER = 2048
SEQ = 16384
EXPERTS = 64
MOE_TOK = 32768
CAP = 5
N_TP = 4


def draw_log_input_gate(key, part):
    key_base = jax.random.fold_in(jax.random.fold_in(key, 3), 0)
    return jnp.clip(jax.random.normal(key_base, (HEADS, SEQ), jnp.float32), -4.0, 4.0)


def draw_forget_gate_logits(key, part):
    subkeys = jax.random.split(jax.random.fold_in(key, 5), 4)
    slow_share = 0.5
    slow_heads = jax.random.uniform(subkeys[0], (HEADS,), jnp.float32) < slow_share
    fast_rate = jnp.exp(jax.random.uniform(subkeys[1], (HEADS,), jnp.float32, math.log(1.0 / 100.0), math.log(1.0 / 30.0)))
    head_rate = jnp.where(slow_heads, 0.5 / SEQ, fast_rate)
    segments = SEQ // MIX_DEV
    factor = jnp.exp(jax.random.uniform(subkeys[2], (segments,), jnp.float32, math.log(0.5), math.log(2.0)))
    factor = jnp.repeat(factor, MIX_DEV, total_repeat_length=SEQ)
    noise = 0.7 * jnp.clip(jax.random.normal(subkeys[3], (HEADS, SEQ), jnp.float32), -3.0, 3.0)
    return -jnp.log(head_rate[:, None] * factor[None, :]) + noise


def draw_extra_log_forget(key, part):
    key_spot, key_level = jax.random.split(jax.random.fold_in(key, 7), 2)
    spots = jax.random.randint(key_spot, (HEADS, 2), 0, SEQ)
    levels = jnp.log(jax.random.uniform(key_level, (HEADS, 2), jnp.float32, 0.5, 0.8))
    spot_hit = spots[:, :, None] == jnp.arange(SEQ)[None, None, :]
    return jnp.sum(jnp.where(spot_hit, levels[:, :, None], 0.0), axis=1)


def block_scale(own_key, extent, shards, low, top_value):
    factor_of = 1.0
    for axis_at, blocks in shards:
        heights = jax.random.uniform(jax.random.fold_in(jax.random.fold_in(own_key, 6), axis_at), (blocks,), jnp.float32, low / len(shards), top_value / len(shards))
        factor_of = factor_of * jnp.repeat(jnp.exp(heights), extent[axis_at] // blocks).reshape((-1,) + (1,) * (len(extent) - 1 - axis_at))
    return factor_of


def deal_out(rng, own, number, rows, number_of, top, limit, lean):
    sequence = jax.random.permutation(rng, number_of)
    packed, ordinary = load_shares(number_of, rows * top, limit, lean, True), load_shares(number_of, rows * top, limit, lean, False)
    places = jnp.arange(number_of)

    def named(sizes, offset_by):
        used = int((sizes > 0).sum())
        fixed = max(1, used // 4)
        moved = fixed + (places - fixed + offset_by * (used - fixed)) % max(1, number_of - fixed)
        return jnp.zeros((number_of,), jnp.int32).at[sequence[jnp.where(places < fixed, places, moved)]].set(jnp.asarray(sizes, jnp.int32))

    sizes = jnp.where(number % 4 == 0, named(packed, number // 4), named(ordinary, number - number // 4 - 1))
    mixed = jax.random.permutation(jax.random.fold_in(own, 3), number_of)
    source_of, taker = mixed[0:number_of // 2 * 2:2], mixed[1:number_of // 2 * 2:2]
    margin = jnp.minimum(sizes[source_of] - 1, limit - sizes[taker]) // 2
    margin = jnp.where((source_of == sequence[0]) | (taker == sequence[0]) | (sizes[taker] == 0), 0, jnp.maximum(margin, 0))
    moved = jax.random.randint(jax.random.fold_in(own, 4), (number_of // 2,), 0, 1 << 20) % (margin + 1)
    sizes = sizes.at[source_of].add(-moved).at[taker].add(moved)
    items = jnp.searchsorted(jnp.cumsum(sizes), jnp.arange(rows * top), side="right").astype(jnp.int32)
    listing = items.reshape(top, rows).T
    listing = listing[jax.random.permutation(jax.random.fold_in(own, 1), rows)]
    offset_by = jax.random.randint(jax.random.fold_in(own, 2), (rows, 1), 0, top)
    return jnp.take_along_axis(listing, (jnp.arange(top)[None, :] + offset_by) % top, axis=1)


def load_shares(amount, total, bound, skew, full):
    weights = [(1 << 20) // math.isqrt(grade ** skew) + 1 for grade in range(1, amount + 1)]
    largest = bound if full else min(bound, max(-(-total // amount), total * weights[0] // sum(weights)))
    least = 1 if total - largest >= amount - 1 else 0
    counts, surplus = [largest] + [least] * (amount - 1), total - largest - least * (amount - 1)
    while surplus > 0:
        candidates = [i for i in range(1, amount) if counts[i] < largest] or [i for i in range(1, amount) if counts[i] < bound]
        mass, budget = sum([weights[i] for i in candidates]), surplus
        for i in candidates:
            more = min(bound - counts[i], max(1, budget * weights[i] // mass), surplus)
            counts[i] = counts[i] + more
            surplus = surplus - more
    return np.array(counts)


def gaussian(stream_key, dims, scale, reach, cuts=(), kind=jnp.bfloat16):
    gain = block_scale(stream_key, dims, cuts, -0.22, 0.18) if cuts else 1.0
    drawn = jax.random.normal(stream_key, dims, jnp.float32) * scale * gain
    return jnp.minimum(jnp.maximum(drawn, -reach), reach).astype(kind)


def setup_inputs(seed: int = 0) -> dict:
    key_list = jax.random.split(jax.random.key(seed), 16)
    cell_query_rows = gaussian(key_list[0], (SEQ, INNER), 1.0, 6.0, ((0, 64), (1, 4)))
    cell_key_rows = gaussian(key_list[1], (SEQ, INNER), 1.0, 6.0, ((0, 64), (1, 4)))
    cell_value_rows = gaussian(key_list[2], (SEQ, INNER), 1.0, 6.0, ((0, 64), (1, 4)))
    output_gate_logits = gaussian(key_list[3], (SEQ, INNER), 1.5, 8.0, ((0, 64), (1, 4)))
    log_input_gate = draw_log_input_gate(jax.random.fold_in(key_list[15], 71), 0)
    forget_gate_logits = draw_forget_gate_logits(jax.random.fold_in(key_list[15], 71), 0)
    extra_log_forget = draw_extra_log_forget(jax.random.fold_in(key_list[15], 71), 0)
    cell_output_scale = jnp.clip(1.0 + 0.18 * jax.random.normal(key_list[7], (INNER,), jnp.float32), 0.1, 1.9)
    tokens_into_experts = gaussian(key_list[8], (MOE_TOK, D), 1.0, 6.0, ((0, 256),))
    expert_norm_scale = jnp.clip(1.0 + 0.18 * jax.random.normal(key_list[9], (D,), jnp.float32), 0.1, 1.9)
    token_expert_index_keys = jax.random.split(jax.random.fold_in(key_list[10], 1), MOE_TOK // MOE_DEV)
    token_expert_index_turns = jax.random.permutation(jax.random.fold_in(key_list[10], 3), MOE_TOK // MOE_DEV)
    token_expert_index = jax.vmap(lambda own, number: deal_out(jax.random.fold_in(key_list[10], 2), own, number, MOE_DEV, EXPERTS, TOPK, CAP, 2))(token_expert_index_keys, token_expert_index_turns).reshape((MOE_TOK, TOPK))
    chosen_expert_weight = jnp.clip(jnp.exp(math.log(3.0) - 2.3025851 * jax.random.uniform(key_list[11], (MOE_TOK, TOPK), jnp.float32) ** block_scale(key_list[11], (MOE_TOK, TOPK), ((0, 256),), -0.2, 0.2)), 0.3, 3.0)
    expert_gate_weight = gaussian(key_list[12], (EXPERTS, D, FF), D ** -0.5, 0.125, ((0, 64), (2, 4)))
    expert_up_weight = gaussian(key_list[13], (EXPERTS, D, FF), D ** -0.5, 0.125, ((0, 64), (2, 4)))
    expert_down_weight = gaussian(key_list[14], (EXPERTS, FF, D), FF ** -0.5, 0.09375, ((0, 64), (1, 4)))
    return dict(cell_query_rows=cell_query_rows, cell_key_rows=cell_key_rows, cell_value_rows=cell_value_rows, output_gate_logits=output_gate_logits, log_input_gate=log_input_gate, forget_gate_logits=forget_gate_logits, extra_log_forget=extra_log_forget, cell_output_scale=cell_output_scale, tokens_into_experts=tokens_into_experts, expert_norm_scale=expert_norm_scale, token_expert_index=token_expert_index, chosen_expert_weight=chosen_expert_weight, expert_gate_weight=expert_gate_weight, expert_up_weight=expert_up_weight, expert_down_weight=expert_down_weight)


EPSILON = 1e-06
PRECISE = lax.Precision.HIGHEST

def mixer_block(running, inputs):
    cell_state, norm_state, stabilizer = running
    queries, key_block, value_block, gate_input, forget_gate_value = inputs
    length = queries.shape[1]
    causal = jnp.tril(jnp.ones((length, length), dtype=bool))
    cumulative = jnp.cumsum(forget_gate_value, axis=-1)
    spread = jnp.where(causal, cumulative[:, :, None] - cumulative[:, None, :] + gate_input[:, None, :], -jnp.inf)
    inter_log = cumulative + stabilizer[:, None]
    row_top = jnp.maximum(inter_log, lax.optimization_barrier(jnp.max(spread, axis=-1)))
    intra_weight = jnp.exp(spread - row_top[:, :, None])
    inter_weight = jnp.exp(inter_log - row_top)
    scores = jnp.einsum('htd,hsd->hts', queries, key_block, precision=PRECISE) * intra_weight
    weights = lax.optimization_barrier(scores.astype(jnp.bfloat16)).astype(jnp.float32)
    numerator = jnp.einsum('hts,hsd->htd', weights, value_block, precision=PRECISE)
    numerator = numerator + inter_weight[:, :, None] * jnp.einsum('hvk,htk->htv', cell_state, queries, precision=PRECISE)
    denominator = lax.optimization_barrier(jnp.sum(scores, axis=-1)) + inter_weight * jnp.einsum('hk,htk->ht', norm_state, queries, precision=PRECISE)
    cell_out = numerator / jnp.maximum(jnp.abs(denominator), 1.0)[:, :, None]
    block_last = cumulative[:, -1]
    growth = block_last[:, None] - cumulative + gate_input
    new_top = jnp.maximum(block_last + stabilizer, lax.optimization_barrier(jnp.max(growth, axis=-1)))
    keep_factor = jnp.exp(block_last + stabilizer - new_top)
    shares = jnp.exp(growth - new_top[:, None])
    cell_state = keep_factor[:, None, None] * cell_state + jnp.einsum('hsv,hsk->hvk', value_block * shares[:, :, None], key_block, precision=PRECISE)
    norm_state = keep_factor[:, None] * norm_state + jnp.einsum('hs,hsk->hk', shares, key_block, precision=PRECISE)
    return ((cell_state, norm_state, new_top), cell_out)

def recurrent_cell_output(cell_query_rows, cell_key_rows, cell_value_rows, output_gate_logits, log_input_gate, forget_gate_logits, extra_log_forget, cell_output_scale):
    seq_len, row_width = cell_query_rows.shape
    head_count = row_width // HEAD_DIM
    block_count = seq_len // BLOCK

    def to_blocks(array):
        return array.astype(jnp.float32).reshape(block_count, BLOCK, head_count, HEAD_DIM).transpose(0, 2, 1, 3)

    def gate_blocks(array):
        return array.reshape(head_count, block_count, BLOCK).transpose(1, 0, 2)
    forget_log_value = jax.nn.log_sigmoid(forget_gate_logits) + extra_log_forget
    start_state = (jnp.zeros((head_count, HEAD_DIM, HEAD_DIM), jnp.float32), jnp.zeros((head_count, HEAD_DIM), jnp.float32), jnp.zeros((head_count,), jnp.float32))
    inputs = (to_blocks(cell_query_rows), to_blocks(cell_key_rows) * HEAD_DIM ** (-0.5), to_blocks(cell_value_rows), gate_blocks(log_input_gate), gate_blocks(forget_log_value))
    _, outputs = lax.scan(mixer_block, start_state, inputs)
    cell_out = outputs.transpose(0, 2, 1, 3).reshape(seq_len, row_width)
    gated = cell_out * cell_output_scale * jax.nn.sigmoid(output_gate_logits.astype(jnp.float32))
    return gated.astype(jnp.bfloat16)

def slot_tables(ids, experts, capacity):
    flat_ids = ids.reshape(-1)
    onehot = (flat_ids[:, None] == jnp.arange(experts, dtype=jnp.int32)[None, :]).astype(jnp.int32)
    earlier = jnp.cumsum(onehot, axis=0) - onehot
    rank_in = lax.optimization_barrier(jnp.sum(earlier * onehot, axis=1))
    slot_index = flat_ids * capacity + rank_in
    token_of = jnp.arange(flat_ids.shape[0], dtype=jnp.int32) // ids.shape[1]
    slot_hit = slot_index[:, None] == jnp.arange(experts * capacity, dtype=jnp.int32)[None, :]
    slot_owner = lax.optimization_barrier(jnp.sum(jnp.where(slot_hit, token_of[:, None] + 1, 0), axis=0)).astype(jnp.int32)
    return (slot_owner, slot_index.reshape(ids.shape).astype(jnp.int32))

def experts_part(tokens_into_experts, expert_norm_scale, token_expert_index, chosen_expert_weight, expert_gate_weight, expert_up_weight, expert_down_weight):
    input_float = tokens_into_experts.astype(jnp.float32)
    normed = (input_float * lax.rsqrt(lax.optimization_barrier(jnp.mean(input_float * input_float, axis=-1, keepdims=True)) + EPSILON) * expert_norm_scale).astype(jnp.bfloat16)
    block_total = MOE_TOK // MOE_DEV
    block_ids = token_expert_index.reshape(block_total, MOE_DEV, TOPK)

    def tables(ids):
        return slot_tables(ids, EXPERTS, CAP)
    slot_owner, slot_index = jax.vmap(tables)(block_ids)
    offsets = jnp.arange(block_total, dtype=jnp.int32) * MOE_DEV
    owner_view = slot_owner.reshape(block_total, EXPERTS, CAP).transpose(1, 0, 2)
    row_index = jnp.where(owner_view > 0, owner_view - 1 + offsets[None, :, None], -1).reshape(EXPERTS, block_total * CAP)
    quarter = FF // N_TP

    def one_expert(inputs):
        index_rows, gate_matrix, up_matrix, down_matrix = inputs
        routed_rows = jnp.where((index_rows >= 0)[:, None], normed[jnp.maximum(index_rows, 0)], jnp.zeros((), jnp.bfloat16))
        gate_out = jnp.dot(routed_rows, gate_matrix, preferred_element_type=jnp.float32)
        up_out = jnp.dot(routed_rows, up_matrix, preferred_element_type=jnp.float32)
        hidden = (jax.nn.silu(gate_out) * up_out).astype(jnp.bfloat16)
        summed = jnp.zeros((routed_rows.shape[0], down_matrix.shape[1]), jnp.float32)
        for group_index in range(N_TP):
            term = jnp.dot(hidden[:, group_index * quarter:(group_index + 1) * quarter], down_matrix[group_index * quarter:(group_index + 1) * quarter], preferred_element_type=jnp.float32).astype(jnp.bfloat16)
            summed = summed + lax.optimization_barrier(term).astype(jnp.float32)
        return summed.astype(jnp.bfloat16)
    results = lax.map(one_expert, (row_index, expert_gate_weight, expert_up_weight, expert_down_weight))
    rank_in = slot_index - block_ids * CAP
    position = jnp.arange(block_total, dtype=jnp.int32)[:, None, None] * CAP + rank_in
    picked = results[block_ids, position]
    weights = chosen_expert_weight.reshape(block_total, MOE_DEV, TOPK)
    combined = lax.optimization_barrier(jnp.sum(weights[..., None] * picked.astype(jnp.float32), axis=2))
    return combined.reshape(MOE_TOK, picked.shape[-1]).astype(jnp.bfloat16)

def reference(cell_query_rows, cell_key_rows, cell_value_rows, output_gate_logits, log_input_gate, forget_gate_logits, extra_log_forget, cell_output_scale, tokens_into_experts, expert_norm_scale, token_expert_index, chosen_expert_weight, expert_gate_weight, expert_up_weight, expert_down_weight):
    gated_head_output = recurrent_cell_output(cell_query_rows, cell_key_rows, cell_value_rows, output_gate_logits, log_input_gate, forget_gate_logits, extra_log_forget, cell_output_scale)
    expert_output = experts_part(tokens_into_experts, expert_norm_scale, token_expert_index, chosen_expert_weight, expert_gate_weight, expert_up_weight, expert_down_weight)
    return (gated_head_output, expert_output)
```

```python
import functools
import math

import jax
import jax.numpy as jnp
from jax import lax
from jax.experimental import pallas as pl
from jax.experimental.pallas import tpu as pltpu
from jax.sharding import Mesh
from jax.sharding import PartitionSpec as P

HEAD_DIM = 256
TOPK = 2
EPSILON = 1e-06
FAR = 1e30
META = 16
GROUPS = ((0, 2), (2, 5))
YC = ("z", "y", "c")
ALL = ("z", "y", "c", "x")
F32 = jnp.float32
BF16 = jnp.bfloat16


VMEM = pl.BlockSpec(memory_space=pltpu.VMEM)
SMEM = pl.BlockSpec(memory_space=pltpu.SMEM)


def call(body, out_shape, in_specs, name, scratch=(), flops=0, limit=16 << 20):
    many = isinstance(out_shape, (list, tuple))
    return pl.pallas_call(
        body,
        out_shape=out_shape,
        in_specs=in_specs,
        out_specs=[VMEM] * len(out_shape) if many else VMEM,
        scratch_shapes=list(scratch),
        name=name,
        cost_estimate=pl.CostEstimate(flops=flops, bytes_accessed=flops // 256, transcendentals=0),
        compiler_params=pltpu.CompilerParams(vmem_limit_bytes=limit),
    )


def shape(dims, dtype=BF16):
    return jax.ShapeDtypeStruct(dims, dtype)


def pack(ref, cell, norm, top, total):
    dim = cell.shape[0]
    dtype = ref.dtype
    ref[0:dim, :] = cell.astype(dtype)
    row = lax.broadcasted_iota(jnp.int32, (META, dim), 0)
    meta = jnp.zeros((META, dim), F32)
    for at, value in enumerate((norm, top, total)):
        value = jnp.broadcast_to(value, (1, dim))
        for term in range(3):
            part = value.astype(BF16).astype(F32)
            value = value - part
            meta = jnp.where(row == 3 * at + term, part, meta)
    ref[dim : dim + META, :] = meta.astype(dtype)


def unpack(ref):
    dim = ref.shape[1]
    meta = ref[dim : dim + META, :].astype(F32)
    values = [meta[3 * k : 3 * k + 1] + meta[3 * k + 1 : 3 * k + 2] + meta[3 * k + 2 : 3 * k + 3] for k in range(3)]
    return values


def matrix(ref):
    return ref[0 : ref.shape[1], :].astype(F32)


def flag(condition):
    return jnp.where(condition, 1.0, 0.0).astype(F32)


def joined(entries, start=None):
    levels = []
    for j, (at, included, _, top, _) in enumerate(entries):
        level = top
        for i, (other_at, other_included, _, _, total) in enumerate(entries):
            if i != j:
                level = level + total * (other_included * flag(other_at > at))
        levels.append(level * included + (included - 1.0) * FAR)
    total_all = sum(entry[4] * entry[1] for entry in entries)
    highest = functools.reduce(jnp.maximum, levels)
    if start is not None:
        highest = jnp.maximum(highest, total_all + start)
    weights = [jnp.exp(level - highest) * entry[1] for level, entry in zip(levels, entries)]
    norm = sum(weight * entry[2] for weight, entry in zip(weights, entries))
    return weights, norm, highest, total_all


def gate_terms(forget_ref, extra_ref, gate_ref, head):
    dim = forget_ref.shape[1]
    logits = forget_ref[pl.ds(head, 1), :]
    log_forget = (
        jnp.minimum(logits, 0.0) - jnp.log1p(jnp.exp(-jnp.abs(logits))) + extra_ref[pl.ds(head, 1), :]
    )
    gate_row = gate_ref[pl.ds(head, 1), :]
    row = lax.broadcasted_iota(jnp.int32, (dim, dim), 0)
    col = lax.broadcasted_iota(jnp.int32, (dim, dim), 1)
    spread = jnp.broadcast_to(log_forget, (dim, dim))
    forget_col = jnp.sum(jnp.where(row == col, spread, 0.0), axis=1, keepdims=True)
    cum_col = jnp.sum(jnp.where(col <= row, spread, 0.0), axis=1, keepdims=True)
    cum_row = jnp.sum(jnp.where(row <= col, forget_col, 0.0), axis=0, keepdims=True)
    gate_col = jnp.sum(jnp.where(row == col, jnp.broadcast_to(gate_row, (dim, dim)), 0.0), axis=1, keepdims=True)
    return cum_col, cum_row, gate_col, gate_row, row, col


def totals_body(where_ref, key_ref, value_ref, gate_ref, forget_ref, extra_ref, own_ref, other_ref):
    core = where_ref[2]
    n_pos = key_ref.shape[0]
    for head, ref in ((core, own_ref), (1 - core, other_ref)):
        cum_col, _, gate_col, _, _, _ = gate_terms(forget_ref, extra_ref, gate_ref, head)
        total = cum_col[n_pos - 1 : n_pos, :]
        growth = total - cum_col + gate_col
        top = jnp.max(growth, axis=0, keepdims=True)
        shares = jnp.exp(growth - top)
        lanes = pl.ds(pl.multiple_of(head * HEAD_DIM, HEAD_DIM), HEAD_DIM)
        keys = key_ref[:, lanes]
        weighted = value_ref[:, lanes].astype(F32) * (shares * HEAD_DIM**-0.5)
        high = weighted.astype(BF16)
        low = (weighted - high.astype(F32)).astype(BF16)
        turned = (((0,), (0,)), ((), ()))
        cell = lax.dot_general(keys, high, turned, preferred_element_type=F32)
        cell = cell + lax.dot_general(keys, low, turned, preferred_element_type=F32)
        norm = jnp.sum(keys.astype(F32) * (shares * HEAD_DIM**-0.5), axis=0, keepdims=True)
        pack(ref, cell, norm, top, total)


def chip_body(where_ref, own_ref, other_ref, out_ref):
    core = where_ref[2]
    entries = [(core, 1.0, *unpack(own_ref)), (1 - core, 1.0, *unpack(other_ref))]
    weights, norm, top, total = joined(entries)
    cell = weights[0] * matrix(own_ref) + weights[1] * matrix(other_ref)
    pack(out_ref, cell, norm, top, total)


def plane_body(count, where_ref, *refs):
    sources, plane_ref, before_ref = refs[:count], refs[count], refs[count + 1]
    me = where_ref[1]
    spots = [lax.rem(me + offset, count) for offset in range(count)]
    states = [unpack(ref) for ref in sources]
    weights, norm, top, total = joined([(at, 1.0, *state) for at, state in zip(spots, states)])
    cell = sum(weight * matrix(ref) for weight, ref in zip(weights, sources))
    pack(plane_ref, cell, norm, top, total)
    weights, norm, top, total = joined([(at, flag(at < me), *state) for at, state in zip(spots, states)])
    cell = sum(weight * matrix(ref) for weight, ref in zip(weights, sources))
    pack(before_ref, cell, norm, top, total)


def prefix_body(count, where_ref, before_ref, own_ref, other_ref, *refs):
    sources, mine_ref, partner_ref = refs[: count - 1], refs[count - 1], refs[count]
    me, core = where_ref[0], where_ref[2]
    spots = [lax.rem(me + offset, count) for offset in range(1, count)]
    entries = [(at, flag(at < me), *unpack(ref)) for at, ref in zip(spots, sources)]
    entries.append((count, 1.0, *unpack(before_ref)))
    own, other, second = unpack(own_ref), unpack(other_ref), core.astype(F32)
    first = [a * (1.0 - second) + b * second for a, b in zip(own, other)]
    first_cell = matrix(own_ref) * (1.0 - second) + matrix(other_ref) * second
    for target, ref in ((core, mine_ref), (1 - core, partner_ref)):
        listed = entries + [(count + 1, target.astype(F32), *first)]
        weights, norm, top, total = joined(listed, start=0.0)
        cell = weights[-1] * first_cell + weights[-2] * matrix(before_ref)
        for weight, source in zip(weights, sources):
            cell = cell + weight * matrix(source)
        pack(ref, cell, norm, top, total)


def outputs_body(
    where_ref,
    query_ref,
    key_ref,
    value_ref,
    open_ref,
    gate_ref,
    forget_ref,
    extra_ref,
    scale_ref,
    own_ref,
    other_ref,
    out_ref,
):
    core = where_ref[2]
    for head, state_ref in ((core, own_ref), (1 - core, other_ref)):
        cum_col, cum_row, _, gate_row, row, col = gate_terms(forget_ref, extra_ref, gate_ref, head)
        norm, top_in, _ = unpack(state_ref)
        dim = state_ref.shape[1]
        lanes = pl.ds(pl.multiple_of(head * HEAD_DIM, HEAD_DIM), HEAD_DIM)
        queries, keys, values = query_ref[:, lanes], key_ref[:, lanes], value_ref[:, lanes]
        inter_log = cum_col + top_in[:, 0:1]
        spread = jnp.where(col <= row, cum_col - cum_row + gate_row, -jnp.inf)
        row_top = jnp.maximum(inter_log, jnp.max(spread, axis=1, keepdims=True))
        inter = jnp.exp(inter_log - row_top)
        scores = lax.dot_general(queries, keys, (((1,), (1,)), ((), ())), preferred_element_type=F32)
        scores = scores * HEAD_DIM**-0.5 * jnp.exp(spread - row_top)
        numerator = jnp.dot(scores.astype(BF16), values, preferred_element_type=F32)
        numerator = numerator + inter * jnp.dot(queries, state_ref[0:dim, :], preferred_element_type=F32)
        met = jnp.sum(queries.astype(F32) * norm, axis=1, keepdims=True)
        denominator = jnp.sum(scores, axis=1, keepdims=True) + inter * met
        cell_out = numerator / jnp.maximum(jnp.abs(denominator), 1.0)
        opened = jax.nn.sigmoid(open_ref[:, lanes].astype(F32))
        out_ref[:, lanes] = (cell_out * scale_ref[:, lanes] * opened).astype(BF16)


def moved(x, axis, shift):
    size = lax.axis_size(axis)
    return lax.ppermute(x, axis, [(k, (k + shift) % size) for k in range(size)])


PACKED = (HEAD_DIM + META, HEAD_DIM)


def chip_state(where, keys, values, gates):
    own, other = call(totals_body, [shape(PACKED)] * 2, [SMEM] + [VMEM] * 5, "cell_totals", flops=1 << 27)(
        where, keys, values, *gates
    )
    other = moved(other, "c", 1)
    chip = call(chip_body, shape(PACKED), [SMEM] + [VMEM] * 2, "cell_chip", flops=1 << 25)(where, own, other)
    return own, other, chip


def plane_state(where, chip):
    wide = lax.axis_size("y")
    chips = [chip] + [moved(chip, "y", -offset) for offset in range(1, wide)]
    return call(
        functools.partial(plane_body, wide),
        [shape(PACKED), shape(PACKED, F32)],
        [SMEM] + [VMEM] * wide,
        "cell_plane",
        flops=1 << 26,
    )(where, *chips)


def entering_state(where, before, own, other, planes):
    high = len(planes) + 1
    mine, partner = call(
        functools.partial(prefix_body, high), [shape(PACKED)] * 2, [SMEM] + [VMEM] * (high + 2), "cell_prefix", flops=1 << 26
    )(where, before, own, other, *planes)
    return mine, moved(partner, "c", 1)


def cell_outputs(where, queries, keys, values, opened, gates, scale, mine, arrived):
    return call(outputs_body, shape(queries.shape), [SMEM] + [VMEM] * 10, "cell_outputs", flops=1 << 28)(
        where, queries, keys, values, opened, *gates, scale.reshape(1, -1), mine, arrived
    )


def places(ids_ref, experts):
    n_tok = ids_ref.shape[0]
    ids = ids_ref[...]
    lane = lax.broadcasted_iota(jnp.int32, (n_tok, experts), 1)
    named = [ids[:, k : k + 1] == lane for k in range(TOPK)]
    both = sum(jnp.where(hit, 1.0, 0.0) for hit in named)
    row = lax.broadcasted_iota(jnp.int32, (n_tok, n_tok), 0)
    col = lax.broadcasted_iota(jnp.int32, (n_tok, n_tok), 1)
    earlier = jnp.where(col < row, 1.0, 0.0).astype(BF16)
    ranks = jnp.dot(earlier, both.astype(BF16), preferred_element_type=F32)
    return [
        (ids[:, k : k + 1], jnp.sum(jnp.where(named[k], ranks, 0.0), axis=1, keepdims=True).astype(jnp.int32))
        for k in range(TOPK)
    ]


def chosen(place, experts, low, high):
    index, rank = place
    per = high - low
    column = jnp.where((rank >= low) & (rank < high), index * per + rank - low, -1)
    lane = lax.broadcasted_iota(jnp.int32, (index.shape[0], experts * per), 1)
    return jnp.where(column == lane, 1.0, 0.0)


def dispatch_body(experts, groups, token_ref, scale_ref, ids_ref, *out_refs):
    tokens = token_ref[...].astype(F32)
    mean = jnp.mean(tokens * tokens, axis=-1, keepdims=True)
    normed = (tokens * lax.rsqrt(mean + EPSILON) * scale_ref[...]).astype(BF16)
    found = places(ids_ref, experts)
    for (low, high), out_ref in zip(groups, out_refs):
        taken = sum(chosen(place, experts, low, high) for place in found).astype(BF16)
        out_ref[...] = lax.dot_general(
            taken, normed, (((0,), (0,)), ((), ())), preferred_element_type=F32
        ).astype(BF16)


def gather_body(experts, low, high, ids_ref, weight_ref, result_ref, *refs):
    out_ref = refs[-1]
    found = places(ids_ref, experts)
    result = result_ref[...]
    total = refs[0][...] if len(refs) > 1 else None
    for k, place in enumerate(found):
        taken = chosen(place, experts, low, high).astype(BF16)
        part = weight_ref[:, k : k + 1] * jnp.dot(taken, result, preferred_element_type=F32)
        total = part if total is None else total + part
    out_ref[...] = total.astype(out_ref.dtype)


def expert_body(own, left, right, far_a, far_b, gate, up, down, *refs):
    outs, rows, sums = refs[:7], refs[7], refs[8]
    count = own.shape[0]
    half = count // 2
    rows[0:count] = own[...]
    rows[count : 2 * count] = left[...]
    rows[2 * count : 3 * count] = right[...]
    rows[3 * count : 3 * count + half] = far_a[...]
    rows[3 * count + half : 4 * count] = far_b[...]
    step = math.gcd(4 * count, 256)

    def one(k, carry):
        at = pl.ds(pl.multiple_of(k * step, step), step)
        x = rows[at, :]
        gate_out = jnp.dot(x, gate[...], preferred_element_type=F32)
        up_out = jnp.dot(x, up[...], preferred_element_type=F32)
        hidden = (gate_out * jax.nn.sigmoid(gate_out) * up_out).astype(BF16)
        sums[at, :] = jnp.dot(hidden, down[...], preferred_element_type=F32).astype(BF16)
        return carry

    lax.fori_loop(0, 4 * count // step, one, 0)
    outs[0][...] = sums[0:count]
    for k in range(6):
        outs[1 + k][...] = sums[count + k * half : count + (k + 1) * half]


def all_rows(block):
    half = block.shape[0] // 2
    from_left = moved(block, "x", 1)
    from_right = moved(block, "x", -1)
    far_a = moved(from_left[:half], "x", 1)
    far_b = moved(from_right[half:], "x", -1)
    return block, from_left, from_right, far_a, far_b


def expert_parts(rows, gate, up, down):
    count, wide = rows[0].shape
    half = count // 2
    return call(
        expert_body,
        [shape((count, wide))] + [shape((half, wide))] * 6,
        [VMEM] * 8,
        "experts",
        scratch=[pltpu.VMEM((4 * count, wide), BF16), pltpu.VMEM((4 * count, wide), BF16)],
        flops=4 * count * 2 * wide * 3 * gate.shape[1],
        limit=34 << 20,
    )(*rows, gate, up, down)


def added(a, b):
    return (a.astype(F32) + b.astype(F32)).astype(BF16)


def summed(parts):
    own, left_a, left_b, right_a, right_b, away_a, away_b = parts
    relay_a = moved(away_a, "x", 1)
    relay_b = moved(away_b, "x", -1)
    low_b = moved(right_b, "x", 1)
    high_a = moved(left_a, "x", -1)
    low_a = moved(added(right_a, relay_a), "x", 1)
    high_b = moved(added(left_b, relay_b), "x", -1)
    low = jnp.concatenate([low_a, low_b]).astype(F32)
    high = jnp.concatenate([high_a, high_b]).astype(F32)
    return (own.astype(F32) + low + high).astype(BF16)


def exchanged(rows, devices):
    wide = rows.shape[1]
    flat = rows.reshape(devices, -1, 128)
    return lax.all_to_all(flat, YC, 0, 0, tiled=True).reshape(-1, wide)


def local(
    cell_query_rows,
    cell_key_rows,
    cell_value_rows,
    output_gate_logits,
    log_input_gate,
    forget_gate_logits,
    extra_log_forget,
    cell_output_scale,
    tokens_into_experts,
    expert_norm_scale,
    token_expert_index,
    chosen_expert_weight,
    expert_gate_weight,
    expert_up_weight,
    expert_down_weight,
):
    where = jnp.stack([lax.axis_index(name) for name in ALL]).astype(jnp.int32)
    gates = (log_input_gate, forget_gate_logits, extra_log_forget)
    experts = lax.axis_size(YC)
    n_tok, wide = tokens_into_experts.shape
    weights = (expert_gate_weight[0], expert_up_weight[0], expert_down_weight[0])
    blocks = call(
        functools.partial(dispatch_body, experts, GROUPS),
        [shape((experts * (high - low), wide)) for low, high in GROUPS],
        [VMEM] * 3,
        "dispatch",
        flops=1 << 28,
    )(tokens_into_experts, expert_norm_scale.reshape(1, -1), token_expert_index)

    def gathered(at, result, *total):
        low, high = GROUPS[at]
        last = at == len(GROUPS) - 1
        return call(
            functools.partial(gather_body, experts, low, high),
            shape((n_tok, wide), BF16 if last else F32),
            [VMEM] * (3 + len(total)),
            "gather",
            flops=1 << 28,
        )(token_expert_index, chosen_expert_weight, result, *total)

    together = lax.optimization_barrier
    first = exchanged(blocks[0], experts)
    own, other, chip = chip_state(where, cell_key_rows, cell_value_rows, gates)
    first, chip = together((first, chip))
    second = exchanged(blocks[1], experts)
    plane, before = plane_state(where, chip)
    first_rows = all_rows(first)
    second, plane = together((second, plane))
    planes = [moved(plane, "z", -offset) for offset in range(1, lax.axis_size("z"))]
    second_rows = all_rows(second)
    first_parts = expert_parts(first_rows, *weights)
    second_parts = expert_parts(second_rows, *weights)
    kept, planes = together((second_parts[0], planes))
    mine, arrived = entering_state(where, before, own, other, planes)
    mixed = cell_outputs(
        where, cell_query_rows, cell_key_rows, cell_value_rows, output_gate_logits, gates, cell_output_scale, mine, arrived
    )
    first_back = exchanged(summed(first_parts), experts)
    second_sum, mixed = together((summed((kept, *second_parts[1:])), mixed))
    second_back = exchanged(second_sum, experts)
    expert_output = gathered(1, second_back, gathered(0, first_back))
    return (mixed, expert_output)


def solution(mesh):
    devices = mesh.devices
    finer = Mesh(devices.reshape(-1, 4, 2, mesh.shape["tp"]), ALL)
    placed = (
        P(YC, "x"),
        P(YC, "x"),
        P(YC, "x"),
        P(YC, "x"),
        P("x", YC),
        P("x", YC),
        P("x", YC),
        P("x"),
        P(ALL, None),
        P(),
        P(ALL, None),
        P(ALL, None),
        P(YC, None, "x"),
        P(YC, None, "x"),
        P(YC, "x", None),
    )
    return jax.shard_map(
        local, mesh=finer, in_specs=placed, out_specs=(P(YC, "x"), P(ALL, None)), check_vma=False
    )
```

```python
import functools

import jax
import jax.numpy as jnp
from jax import lax
from jax.experimental import pallas as pl
from jax.experimental.pallas import tpu as pltpu
from jax.sharding import Mesh
from jax.sharding import PartitionSpec as P


HEAD_DIM = 256
TOPK = 2
EPSILON = 1e-06
FAR = 1e30
META = 16
LANES = 128
EXPERT_LIMIT = 30 << 20
PACKED = (256 + META, 256)
GROUPS = ((0, 3), (3, 5))
YC = ("z", "y", "c")
ALL = ("z", "y", "c", "x")
F32 = jnp.float32
BF16 = jnp.bfloat16


VMEM = pl.BlockSpec(memory_space=pltpu.VMEM)
SMEM = pl.BlockSpec(memory_space=pltpu.SMEM)


def call(body, out_shape, in_specs, scratch=(), flops=0, limit=16 << 20):
    many = isinstance(out_shape, (list, tuple))
    return pl.pallas_call(
        body,
        out_shape=out_shape,
        in_specs=in_specs,
        out_specs=[VMEM] * len(out_shape) if many else VMEM,
        scratch_shapes=list(scratch),
        cost_estimate=pl.CostEstimate(flops=flops, bytes_accessed=flops // 256, transcendentals=0),
        compiler_params=pltpu.CompilerParams(vmem_limit_bytes=limit),
    )


def shape(dims, dtype=BF16):
    return jax.ShapeDtypeStruct(dims, dtype)


def pack(ref, cell, norm, top, total):
    dim = cell.shape[0]
    dtype = ref.dtype
    ref[0:dim, :] = cell.astype(dtype)
    row = lax.broadcasted_iota(jnp.int32, (META, dim), 0)
    meta = jnp.zeros((META, dim), F32)
    for at, value in enumerate((norm, top, total)):
        value = jnp.broadcast_to(value, (1, dim))
        for term in range(3):
            part = value.astype(BF16).astype(F32)
            value = value - part
            meta = jnp.where(row == 3 * at + term, part, meta)
    ref[dim : dim + META, :] = meta.astype(dtype)


def unpack(ref):
    dim = ref.shape[1]
    meta = ref[dim : dim + META, :].astype(F32)
    values = [meta[3 * k : 3 * k + 1] + meta[3 * k + 1 : 3 * k + 2] + meta[3 * k + 2 : 3 * k + 3] for k in range(3)]
    return values


def matrix(ref):
    return ref[0 : ref.shape[1], :].astype(F32)


def flag(condition):
    return jnp.where(condition, 1.0, 0.0).astype(F32)


def joined(entries, start=None):
    levels = []
    for j, (at, included, _, top, _) in enumerate(entries):
        level = top
        for i, (other_at, other_included, _, _, total) in enumerate(entries):
            if i != j:
                level = level + total * (other_included * flag(other_at > at))
        levels.append(level * included + (included - 1.0) * FAR)
    total_all = sum(entry[4] * entry[1] for entry in entries)
    highest = functools.reduce(jnp.maximum, levels)
    if start is not None:
        highest = jnp.maximum(highest, total_all + start)
    weights = [jnp.exp(level - highest) * entry[1] for level, entry in zip(levels, entries)]
    norm = sum(weight * entry[2] for weight, entry in zip(weights, entries))
    return weights, norm, highest, total_all


def gate_terms(forget_ref, extra_ref, gate_ref, head):
    dim = forget_ref.shape[1]
    logits = forget_ref[pl.ds(head, 1), :]
    log_forget = (
        jnp.minimum(logits, 0.0) - jnp.log1p(jnp.exp(-jnp.abs(logits))) + extra_ref[pl.ds(head, 1), :]
    )
    gate_row = gate_ref[pl.ds(head, 1), :]
    row = lax.broadcasted_iota(jnp.int32, (dim, dim), 0)
    col = lax.broadcasted_iota(jnp.int32, (dim, dim), 1)
    spread = jnp.broadcast_to(log_forget, (dim, dim))
    forget_col = jnp.sum(jnp.where(row == col, spread, 0.0), axis=1, keepdims=True)
    cum_col = jnp.sum(jnp.where(col <= row, spread, 0.0), axis=1, keepdims=True)
    cum_row = jnp.sum(jnp.where(row <= col, forget_col, 0.0), axis=0, keepdims=True)
    gate_col = jnp.sum(jnp.where(row == col, jnp.broadcast_to(gate_row, (dim, dim)), 0.0), axis=1, keepdims=True)
    return cum_col, cum_row, gate_col, gate_row, row, col


def totals_body(where_ref, key_ref, value_ref, gate_ref, forget_ref, extra_ref, own_ref, other_ref):
    core = where_ref[2]
    n_pos = key_ref.shape[0]
    for head, ref in ((core, own_ref), (1 - core, other_ref)):
        cum_col, _, gate_col, _, _, _ = gate_terms(forget_ref, extra_ref, gate_ref, head)
        total = cum_col[n_pos - 1 : n_pos, :]
        growth = total - cum_col + gate_col
        top = jnp.max(growth, axis=0, keepdims=True)
        shares = jnp.exp(growth - top)
        lanes = pl.ds(pl.multiple_of(head * HEAD_DIM, HEAD_DIM), HEAD_DIM)
        keys = key_ref[:, lanes]
        weighted = value_ref[:, lanes].astype(F32) * (shares * HEAD_DIM**-0.5)
        high = weighted.astype(BF16)
        low = (weighted - high.astype(F32)).astype(BF16)
        turned = (((0,), (0,)), ((), ()))
        cell = lax.dot_general(keys, high, turned, preferred_element_type=F32)
        cell = cell + lax.dot_general(keys, low, turned, preferred_element_type=F32)
        norm = jnp.sum(keys.astype(F32) * (shares * HEAD_DIM**-0.5), axis=0, keepdims=True)
        pack(ref, cell, norm, top, total)


def chip_body(where_ref, own_ref, other_ref, sent_ref, kept_ref):
    core = where_ref[2]
    entries = [(core, 1.0, *unpack(own_ref)), (1 - core, 1.0, *unpack(other_ref))]
    weights, norm, top, total = joined(entries)
    cell = weights[0] * matrix(own_ref) + weights[1] * matrix(other_ref)
    for ref in (sent_ref, kept_ref):
        pack(ref, cell, norm, top, total)


def earlier_states(upper, got_ref, before_refs):
    listed = [(0, flag(upper == 1), *unpack(got_ref))]
    return listed + [(1, 1.0, *unpack(ref)) for ref in before_refs]


def double_body(axis, bit, where_ref, got_ref, whole_ref, *refs):
    before_refs, (sent_ref, kept_ref, before_out) = refs[:-3], refs[-3:]
    upper = (where_ref[axis] >> bit) & 1
    entries = [(upper, 1.0, *unpack(whole_ref)), (1 - upper, 1.0, *unpack(got_ref))]
    weights, norm, top, total = joined(entries)
    cell = weights[0] * matrix(whole_ref) + weights[1] * matrix(got_ref)
    for ref in (sent_ref, kept_ref):
        pack(ref, cell, norm, top, total)
    weights, norm, top, total = joined(earlier_states(upper, got_ref, before_refs))
    cell = sum(weight * matrix(ref) for weight, ref in zip(weights, (got_ref, *before_refs)))
    pack(before_out, cell, norm, top, total)


def prefix_body(axis, bit, where_ref, got_ref, before_ref, own_ref, other_ref, mine_ref, partner_ref):
    upper, core = (where_ref[axis] >> bit) & 1, where_ref[2]
    own, other, second = unpack(own_ref), unpack(other_ref), core.astype(F32)
    first = [a * (1.0 - second) + b * second for a, b in zip(own, other)]
    first_cell = matrix(own_ref) * (1.0 - second) + matrix(other_ref) * second
    for target, ref in ((core, mine_ref), (1 - core, partner_ref)):
        listed = earlier_states(upper, got_ref, (before_ref,)) + [(2, target.astype(F32), *first)]
        weights, norm, top, total = joined(listed, start=0.0)
        cell = weights[0] * matrix(got_ref) + weights[1] * matrix(before_ref) + weights[2] * first_cell
        pack(ref, cell, norm, top, total)


def outputs_body(
    where_ref,
    query_ref,
    key_ref,
    value_ref,
    open_ref,
    gate_ref,
    forget_ref,
    extra_ref,
    scale_ref,
    own_ref,
    other_ref,
    out_ref,
):
    core = where_ref[2]
    for head, state_ref in ((core, own_ref), (1 - core, other_ref)):
        cum_col, cum_row, _, gate_row, row, col = gate_terms(forget_ref, extra_ref, gate_ref, head)
        norm, top_in, _ = unpack(state_ref)
        dim = state_ref.shape[1]
        lanes = pl.ds(pl.multiple_of(head * HEAD_DIM, HEAD_DIM), HEAD_DIM)
        queries, keys, values = query_ref[:, lanes], key_ref[:, lanes], value_ref[:, lanes]
        inter_log = cum_col + top_in[:, 0:1]
        spread = jnp.where(col <= row, cum_col - cum_row + gate_row, -jnp.inf)
        row_top = jnp.maximum(inter_log, jnp.max(spread, axis=1, keepdims=True))
        inter = jnp.exp(inter_log - row_top)
        scores = lax.dot_general(queries, keys, (((1,), (1,)), ((), ())), preferred_element_type=F32)
        scores = scores * HEAD_DIM**-0.5 * jnp.exp(spread - row_top)
        numerator = jnp.dot(scores.astype(BF16), values, preferred_element_type=F32)
        numerator = numerator + inter * jnp.dot(queries, state_ref[0:dim, :], preferred_element_type=F32)
        met = jnp.sum(queries.astype(F32) * norm, axis=1, keepdims=True)
        denominator = jnp.sum(scores, axis=1, keepdims=True) + inter * met
        cell_out = numerator / jnp.maximum(jnp.abs(denominator), 1.0)
        opened = jax.nn.sigmoid(open_ref[:, lanes].astype(F32))
        out_ref[:, lanes] = (cell_out * scale_ref[:, lanes] * opened).astype(BF16)


def moved(x, axis, shift):
    size = lax.axis_size(axis)
    return lax.ppermute(x, axis, [(k, (k + shift) % size) for k in range(size)])


def flipped(x, axis, bit):
    return lax.ppermute(x, axis, [(k, k ^ (1 << bit)) for k in range(lax.axis_size(axis))])


def places(ids_ref, experts):
    n_tok = ids_ref.shape[0]
    ids = ids_ref[...]
    lane = lax.broadcasted_iota(jnp.int32, (n_tok, experts), 1)
    named = [ids[:, k : k + 1] == lane for k in range(TOPK)]
    both = sum(jnp.where(hit, 1.0, 0.0) for hit in named)
    row = lax.broadcasted_iota(jnp.int32, (n_tok, n_tok), 0)
    col = lax.broadcasted_iota(jnp.int32, (n_tok, n_tok), 1)
    earlier = jnp.where(col < row, 1.0, 0.0).astype(BF16)
    ranks = jnp.dot(earlier, both.astype(BF16), preferred_element_type=F32)
    return [
        (ids[:, k : k + 1], jnp.sum(jnp.where(named[k], ranks, 0.0), axis=1, keepdims=True).astype(jnp.int32))
        for k in range(TOPK)
    ]


def chosen(place, experts, low, high):
    index, rank = place
    per = high - low
    column = jnp.where((rank >= low) & (rank < high), index * per + rank - low, -1)
    lane = lax.broadcasted_iota(jnp.int32, (index.shape[0], experts * per), 1)
    return jnp.where(column == lane, 1.0, 0.0)


def dispatch_body(experts, groups, token_ref, scale_ref, ids_ref, *out_refs):
    tokens = token_ref[...].astype(F32)
    mean = jnp.mean(tokens * tokens, axis=-1, keepdims=True)
    normed = (tokens * lax.rsqrt(mean + EPSILON) * scale_ref[...]).astype(BF16)
    found = places(ids_ref, experts)
    for (low, high), out_ref in zip(groups, out_refs):
        taken = sum(chosen(place, experts, low, high) for place in found).astype(BF16)
        out_ref[...] = lax.dot_general(
            taken, normed, (((0,), (0,)), ((), ())), preferred_element_type=F32
        ).astype(BF16)


def gather_body(experts, low, high, ids_ref, weight_ref, result_ref, *refs):
    out_ref = refs[-1]
    found = places(ids_ref, experts)
    result = result_ref[...]
    total = refs[0][...] if len(refs) > 1 else None
    for k, place in enumerate(found):
        taken = chosen(place, experts, low, high).astype(BF16)
        part = weight_ref[:, k : k + 1] * jnp.dot(taken, result, preferred_element_type=F32)
        total = part if total is None else total + part
    out_ref[...] = total.astype(out_ref.dtype)


def expert_body(own, left, right, far, gate, up, down, *refs):
    outs, (rows, hidden, pairs, held, arrived) = refs[:4], refs[4:]
    count = own.shape[0]
    tiles = gate.shape[1] // LANES

    def halves(j):
        return [
            pltpu.make_async_copy(
                ref.at[:, pl.ds(pl.multiple_of(j * LANES, LANES), LANES)],
                pairs.at[:, pl.ds(pl.multiple_of((2 * j + k) * LANES, LANES), LANES)],
                arrived.at[2 * j + k],
            )
            for k, ref in enumerate((gate, up))
        ]

    last = pltpu.make_async_copy(down, held, arrived.at[2 * tiles])
    for j in range(tiles):
        for copy in halves(j):
            copy.start()
    last.start()
    for k, ref in enumerate((own, left, right, far)):
        rows[k * count : (k + 1) * count] = ref[...]

    def into(j, carry):
        for copy in halves(j):
            copy.wait()
        both = pairs[:, pl.ds(pl.multiple_of(2 * j * LANES, 2 * LANES), 2 * LANES)]
        both = jnp.dot(rows[...], both, preferred_element_type=F32)
        gate_out, up_out = both[:, :LANES], both[:, LANES:]
        columns = pl.ds(pl.multiple_of(j * LANES, LANES), LANES)
        hidden[:, columns] = (gate_out * jax.nn.sigmoid(gate_out) * up_out).astype(BF16)
        return carry

    lax.fori_loop(0, tiles, into, 0)
    last.wait()

    def out_of(j, carry):
        columns = pl.ds(pl.multiple_of(2 * j * LANES, 2 * LANES), 2 * LANES)
        result = jnp.dot(hidden[...], held[:, columns], preferred_element_type=F32).astype(BF16)
        for k, out in enumerate(outs):
            out[:, columns] = result[k * count : (k + 1) * count]
        return carry

    lax.fori_loop(0, down.shape[1] // (2 * LANES), out_of, 0)


def all_rows(block, way):
    from_left = moved(block, "x", 1)
    from_right = moved(block, "x", -1)
    far = moved(from_left if way > 0 else from_right, "x", way)
    return block, from_left, from_right, far


def expert_parts(rows, weights):
    count, wide = rows[0].shape
    part = weights[0].shape[1]
    return call(
        expert_body,
        [shape((count, wide))] * 4,
        [VMEM] * 4 + [pl.BlockSpec(memory_space=pltpu.HBM)] * 3,
        scratch=[
            pltpu.VMEM((4 * count, wide), BF16),
            pltpu.VMEM((4 * count, part), BF16),
            pltpu.VMEM((wide, 2 * part), BF16),
            pltpu.VMEM((part, wide), BF16),
            pltpu.SemaphoreType.DMA((2 * part // LANES + 1,)),
        ],
        flops=4 * count * 2 * wide * 3 * weights[0].shape[1],
        limit=EXPERT_LIMIT,
    )(*rows, *weights)


def added(*terms):
    return functools.reduce(jnp.add, [term.astype(F32) for term in terms]).astype(BF16)


def summed(parts, way):
    own, left, right, away = parts
    relay = moved(away, "x", way)
    low = moved(added(right, relay) if way > 0 else right, "x", 1)
    high = moved(left if way > 0 else added(left, relay), "x", -1)
    return added(own, low, high)


def exchanged(rows, devices):
    wide = rows.shape[1]
    flat = rows.reshape(devices, -1, 128)
    flat = lax.all_to_all(flat, YC, 0, 0, tiled=True)
    return flat.reshape(-1, wide)


def step(
    cell_query_rows,
    cell_key_rows,
    cell_value_rows,
    output_gate_logits,
    log_input_gate,
    forget_gate_logits,
    extra_log_forget,
    cell_output_scale,
    tokens_into_experts,
    expert_norm_scale,
    token_expert_index,
    chosen_expert_weight,
    expert_gate_weight,
    expert_up_weight,
    expert_down_weight,
):
    where = jnp.stack([lax.axis_index(name) for name in ALL]).astype(jnp.int32)
    gates = (log_input_gate, forget_gate_logits, extra_log_forget)
    experts = lax.axis_size(YC)
    n_tok, wide = tokens_into_experts.shape
    weights = (expert_gate_weight[0], expert_up_weight[0], expert_down_weight[0])
    blocks = call(
        functools.partial(dispatch_body, experts, GROUPS),
        [shape((experts * (high - low), wide)) for low, high in GROUPS],
        [VMEM] * 3,
        flops=1 << 28,
    )(tokens_into_experts, expert_norm_scale.reshape(1, -1), token_expert_index)

    def gathered(at, result, *total):
        low, high = GROUPS[at]
        last = at == len(GROUPS) - 1
        return call(
            functools.partial(gather_body, experts, low, high),
            shape((n_tok, wide), BF16 if last else F32),
            [VMEM] * (3 + len(total)),
            flops=1 << 28,
        )(token_expert_index, chosen_expert_weight, result, *total)

    packed, packed_wide = shape(PACKED), shape(PACKED, F32)
    first = exchanged(blocks[0], experts)
    own, other = call(totals_body, [packed] * 2, [SMEM] + [VMEM] * 5, flops=1 << 27)(
        where, cell_key_rows, cell_value_rows, *gates
    )
    other = flipped(other, "c", 0)
    sent, whole = call(chip_body, [packed, packed_wide], [SMEM] + [VMEM] * 2, flops=1 << 25)(where, own, other)
    before = ()
    bits = [(axis, bit) for axis in "yz" for bit in range(lax.axis_size(axis).bit_length() - 1)]
    for axis, bit in bits[:-1]:
        got = flipped(sent, axis, bit)
        sent, whole, *before = call(
            functools.partial(double_body, ALL.index(axis), bit),
            [packed, packed_wide, packed_wide],
            [SMEM] + [VMEM] * (2 + len(before)),
            flops=1 << 25,
        )(where, got, whole, *before)
    axis, bit = bits[-1]
    got = flipped(sent, axis, bit)
    mine, partner = call(
        functools.partial(prefix_body, ALL.index(axis), bit), [packed] * 2, [SMEM] + [VMEM] * 4, flops=1 << 26
    )(where, got, *before, own, other)
    arrived = flipped(partner, "c", 0)
    mixed = call(outputs_body, shape(cell_query_rows.shape), [SMEM] + [VMEM] * 10, flops=1 << 28)(
        where,
        cell_query_rows,
        cell_key_rows,
        cell_value_rows,
        output_gate_logits,
        *gates,
        cell_output_scale.reshape(1, -1),
        mine,
        arrived,
    )
    second = exchanged(blocks[1], experts)
    weights = [pltpu.with_memory_space_constraint(x, pltpu.HBM) for x in weights]
    sums = []
    for block, way in ((first, 1), (second, -1)):
        parts = expert_parts(all_rows(block, way), weights)
        sums.append(summed(parts, way))
    first_back = exchanged(sums[0], experts)
    second_back = exchanged(sums[1], experts)
    expert_output = gathered(1, second_back, gathered(0, first_back))
    return (mixed, expert_output)


def solution(mesh):
    devices = mesh.devices
    finer = Mesh(devices.reshape(-1, 4, 2, mesh.shape["tp"]), ALL)
    placed = (
        P(YC, "x"),
        P(YC, "x"),
        P(YC, "x"),
        P(YC, "x"),
        P("x", YC),
        P("x", YC),
        P("x", YC),
        P("x"),
        P(ALL, None),
        P(),
        P(ALL, None),
        P(ALL, None),
        P(YC, None, "x"),
        P(YC, None, "x"),
        P(YC, "x", None),
    )
    return jax.shard_map(step, mesh=finer, in_specs=placed, out_specs=(P(YC, "x"), P(ALL, None)), check_vma=False)
```

```python
import functools

import jax
import jax.numpy as jnp
from jax import lax
from jax.experimental import pallas as pl
from jax.experimental.pallas import tpu as pltpu
from jax.sharding import Mesh
from jax.sharding import PartitionSpec as P


HEAD_DIM = 256
TOPK = 2
EPSILON = 1e-06
FAR = 1e30
META = 16
LANES = 128
EXPERT_LIMIT = 16 << 20
JOIN_FLOPS = 1 << 33
PACKED = (256 + META, 256)
GROUPS = ((0, 2), (2, 5))
WAYS = (1, 0)
YC = ("z", "y", "c")
ALL = ("z", "y", "c", "x")
F32 = jnp.float32
BF16 = jnp.bfloat16


VMEM = pl.BlockSpec(memory_space=pltpu.VMEM)
SMEM = pl.BlockSpec(memory_space=pltpu.SMEM)


def call(body, out_shape, in_specs, scratch=(), flops=0, limit=16 << 20):
    many = isinstance(out_shape, (list, tuple))
    return pl.pallas_call(
        body,
        out_shape=out_shape,
        in_specs=in_specs,
        out_specs=[VMEM] * len(out_shape) if many else VMEM,
        scratch_shapes=list(scratch),
        cost_estimate=pl.CostEstimate(flops=flops, bytes_accessed=flops // 256, transcendentals=0),
        compiler_params=pltpu.CompilerParams(vmem_limit_bytes=limit),
    )


def shape(dims, dtype=BF16):
    return jax.ShapeDtypeStruct(dims, dtype)


def pack(ref, cell, norm, top, total):
    dim = cell.shape[0]
    dtype = ref.dtype
    ref[0:dim, :] = cell.astype(dtype)
    row = lax.broadcasted_iota(jnp.int32, (META, dim), 0)
    meta = jnp.zeros((META, dim), F32)
    for at, value in enumerate((norm, top, total)):
        value = jnp.broadcast_to(value, (1, dim))
        for term in range(3):
            part = value.astype(BF16).astype(F32)
            value = value - part
            meta = jnp.where(row == 3 * at + term, part, meta)
    ref[dim : dim + META, :] = meta.astype(dtype)


def unpack(ref):
    dim = ref.shape[1]
    meta = ref[dim : dim + META, :].astype(F32)
    values = [meta[3 * k : 3 * k + 1] + meta[3 * k + 1 : 3 * k + 2] + meta[3 * k + 2 : 3 * k + 3] for k in range(3)]
    return values


def matrix(ref):
    return ref[0 : ref.shape[1], :].astype(F32)


def flag(condition):
    return jnp.where(condition, 1.0, 0.0).astype(F32)


def joined(entries, start=None):
    levels = []
    for j, (at, included, _, top, _) in enumerate(entries):
        level = top
        for i, (other_at, other_included, _, _, total) in enumerate(entries):
            if i != j:
                level = level + total * (other_included * flag(other_at > at))
        levels.append(level * included + (included - 1.0) * FAR)
    total_all = sum(entry[4] * entry[1] for entry in entries)
    highest = functools.reduce(jnp.maximum, levels)
    if start is not None:
        highest = jnp.maximum(highest, total_all + start)
    weights = [jnp.exp(level - highest) * entry[1] for level, entry in zip(levels, entries)]
    norm = sum(weight * entry[2] for weight, entry in zip(weights, entries))
    return weights, norm, highest, total_all


def gate_terms(forget_ref, extra_ref, gate_ref, head):
    dim = forget_ref.shape[1]
    logits = forget_ref[pl.ds(head, 1), :]
    log_forget = (
        jnp.minimum(logits, 0.0) - jnp.log1p(jnp.exp(-jnp.abs(logits))) + extra_ref[pl.ds(head, 1), :]
    )
    gate_row = gate_ref[pl.ds(head, 1), :]
    row = lax.broadcasted_iota(jnp.int32, (dim, dim), 0)
    col = lax.broadcasted_iota(jnp.int32, (dim, dim), 1)
    spread = jnp.broadcast_to(log_forget, (dim, dim))
    forget_col = jnp.sum(jnp.where(row == col, spread, 0.0), axis=1, keepdims=True)
    cum_col = jnp.sum(jnp.where(col <= row, spread, 0.0), axis=1, keepdims=True)
    cum_row = jnp.sum(jnp.where(row <= col, forget_col, 0.0), axis=0, keepdims=True)
    gate_col = jnp.sum(jnp.where(row == col, jnp.broadcast_to(gate_row, (dim, dim)), 0.0), axis=1, keepdims=True)
    return cum_col, cum_row, gate_col, gate_row, row, col


def totals_body(where_ref, key_ref, value_ref, gate_ref, forget_ref, extra_ref, own_ref, other_ref):
    core = where_ref[2]
    n_pos = key_ref.shape[0]
    for head, ref in ((core, own_ref), (1 - core, other_ref)):
        cum_col, _, gate_col, _, _, _ = gate_terms(forget_ref, extra_ref, gate_ref, head)
        total = cum_col[n_pos - 1 : n_pos, :]
        growth = total - cum_col + gate_col
        top = jnp.max(growth, axis=0, keepdims=True)
        shares = jnp.exp(growth - top)
        lanes = pl.ds(pl.multiple_of(head * HEAD_DIM, HEAD_DIM), HEAD_DIM)
        keys = key_ref[:, lanes]
        weighted = value_ref[:, lanes].astype(F32) * (shares * HEAD_DIM**-0.5)
        high = weighted.astype(BF16)
        low = (weighted - high.astype(F32)).astype(BF16)
        turned = (((0,), (0,)), ((), ()))
        cell = lax.dot_general(keys, high, turned, preferred_element_type=F32)
        cell = cell + lax.dot_general(keys, low, turned, preferred_element_type=F32)
        norm = jnp.sum(keys.astype(F32) * (shares * HEAD_DIM**-0.5), axis=0, keepdims=True)
        pack(ref, cell, norm, top, total)


def chip_body(where_ref, own_ref, other_ref, sent_ref, kept_ref):
    core = where_ref[2]
    entries = [(core, 1.0, *unpack(own_ref)), (1 - core, 1.0, *unpack(other_ref))]
    weights, norm, top, total = joined(entries)
    cell = weights[0] * matrix(own_ref) + weights[1] * matrix(other_ref)
    for ref in (sent_ref, kept_ref):
        pack(ref, cell, norm, top, total)


def earlier_states(upper, got_ref, before_refs):
    listed = [(0, flag(upper == 1), *unpack(got_ref))]
    return listed + [(1, 1.0, *unpack(ref)) for ref in before_refs]


def double_body(axis, bit, where_ref, got_ref, whole_ref, *refs):
    before_refs, (sent_ref, kept_ref, before_out) = refs[:-3], refs[-3:]
    upper = (where_ref[axis] >> bit) & 1
    entries = [(upper, 1.0, *unpack(whole_ref)), (1 - upper, 1.0, *unpack(got_ref))]
    weights, norm, top, total = joined(entries)
    cell = weights[0] * matrix(whole_ref) + weights[1] * matrix(got_ref)
    for ref in (sent_ref, kept_ref):
        pack(ref, cell, norm, top, total)
    weights, norm, top, total = joined(earlier_states(upper, got_ref, before_refs))
    cell = sum(weight * matrix(ref) for weight, ref in zip(weights, (got_ref, *before_refs)))
    pack(before_out, cell, norm, top, total)


def prefix_body(axis, bit, where_ref, got_ref, before_ref, own_ref, other_ref, mine_ref, partner_ref):
    upper, core = (where_ref[axis] >> bit) & 1, where_ref[2]
    own, other, second = unpack(own_ref), unpack(other_ref), core.astype(F32)
    first = [a * (1.0 - second) + b * second for a, b in zip(own, other)]
    first_cell = matrix(own_ref) * (1.0 - second) + matrix(other_ref) * second
    for target, ref in ((core, mine_ref), (1 - core, partner_ref)):
        listed = earlier_states(upper, got_ref, (before_ref,)) + [(2, target.astype(F32), *first)]
        weights, norm, top, total = joined(listed, start=0.0)
        cell = weights[0] * matrix(got_ref) + weights[1] * matrix(before_ref) + weights[2] * first_cell
        pack(ref, cell, norm, top, total)


def outputs_body(
    where_ref,
    query_ref,
    key_ref,
    value_ref,
    open_ref,
    gate_ref,
    forget_ref,
    extra_ref,
    scale_ref,
    own_ref,
    other_ref,
    out_ref,
):
    core = where_ref[2]
    for head, state_ref in ((core, own_ref), (1 - core, other_ref)):
        cum_col, cum_row, _, gate_row, row, col = gate_terms(forget_ref, extra_ref, gate_ref, head)
        norm, top_in, _ = unpack(state_ref)
        dim = state_ref.shape[1]
        lanes = pl.ds(pl.multiple_of(head * HEAD_DIM, HEAD_DIM), HEAD_DIM)
        queries, keys, values = query_ref[:, lanes], key_ref[:, lanes], value_ref[:, lanes]
        inter_log = cum_col + top_in[:, 0:1]
        spread = jnp.where(col <= row, cum_col - cum_row + gate_row, -jnp.inf)
        row_top = jnp.maximum(inter_log, jnp.max(spread, axis=1, keepdims=True))
        inter = jnp.exp(inter_log - row_top)
        scores = lax.dot_general(queries, keys, (((1,), (1,)), ((), ())), preferred_element_type=F32)
        scores = scores * HEAD_DIM**-0.5 * jnp.exp(spread - row_top)
        numerator = jnp.dot(scores.astype(BF16), values, preferred_element_type=F32)
        numerator = numerator + inter * jnp.dot(queries, state_ref[0:dim, :], preferred_element_type=F32)
        met = jnp.sum(queries.astype(F32) * norm, axis=1, keepdims=True)
        denominator = jnp.sum(scores, axis=1, keepdims=True) + inter * met
        cell_out = numerator / jnp.maximum(jnp.abs(denominator), 1.0)
        opened = jax.nn.sigmoid(open_ref[:, lanes].astype(F32))
        out_ref[:, lanes] = (cell_out * scale_ref[:, lanes] * opened).astype(BF16)


def moved(x, axis, shift):
    size = lax.axis_size(axis)
    return lax.ppermute(x, axis, [(k, (k + shift) % size) for k in range(size)])


def flipped(x, axis, bit):
    return lax.ppermute(x, axis, [(k, k ^ (1 << bit)) for k in range(lax.axis_size(axis))])


def upright(row_values):
    count = row_values.shape[1]
    row = lax.broadcasted_iota(jnp.int32, (count, count), 0)
    col = lax.broadcasted_iota(jnp.int32, (count, count), 1)
    spread = jnp.broadcast_to(row_values, (count, count))
    return jnp.sum(jnp.where(row == col, spread, 0.0), axis=1, keepdims=True)


def places(ids_ref, experts):
    n_tok = ids_ref.shape[1]
    ids = [upright(ids_ref[k : k + 1, :].astype(F32)).astype(jnp.int32) for k in range(TOPK)]
    lane = lax.broadcasted_iota(jnp.int32, (n_tok, experts), 1)
    named = [index == lane for index in ids]
    both = sum(jnp.where(hit, 1.0, 0.0) for hit in named)
    row = lax.broadcasted_iota(jnp.int32, (n_tok, n_tok), 0)
    col = lax.broadcasted_iota(jnp.int32, (n_tok, n_tok), 1)
    earlier = jnp.where(col < row, 1.0, 0.0).astype(BF16)
    ranks = jnp.dot(earlier, both.astype(BF16), preferred_element_type=F32)
    return [
        (index, jnp.sum(jnp.where(hit, ranks, 0.0), axis=1, keepdims=True).astype(jnp.int32))
        for index, hit in zip(ids, named)
    ]


def chosen(place, experts, low, high):
    index, rank = place
    per = high - low
    column = jnp.where((rank >= low) & (rank < high), index * per + rank - low, -1)
    lane = lax.broadcasted_iota(jnp.int32, (index.shape[0], experts * per), 1)
    return jnp.where(column == lane, 1.0, 0.0)


def dispatch_body(experts, groups, token_ref, scale_ref, ids_ref, *refs):
    out_refs, (held, scale, arrived) = refs[: len(groups)], refs[len(groups) :]
    copies = [
        pltpu.make_async_copy(token_ref, held, arrived.at[0]),
        pltpu.make_async_copy(scale_ref, scale, arrived.at[1]),
    ]
    for copy in copies:
        copy.start()
    found = places(ids_ref, experts)
    for copy in copies:
        copy.wait()
    tokens = held[...].astype(F32)
    mean = jnp.mean(tokens * tokens, axis=-1, keepdims=True)
    normed = (tokens * lax.rsqrt(mean + EPSILON) * scale[...]).astype(BF16)
    for (low, high), out_ref in zip(groups, out_refs):
        taken = sum(chosen(place, experts, low, high) for place in found).astype(BF16)
        out_ref[...] = lax.dot_general(
            taken, normed, (((0,), (0,)), ((), ())), preferred_element_type=F32
        ).astype(BF16)


def gather_body(experts, low, high, ids_ref, weight_ref, result_ref, *refs):
    out_ref = refs[-1]
    found = places(ids_ref, experts)
    result = result_ref[...]
    total = refs[0][...] if len(refs) > 1 else None
    for k, place in enumerate(found):
        taken = chosen(place, experts, low, high).astype(BF16)
        part = upright(weight_ref[k : k + 1, :]) * jnp.dot(taken, result, preferred_element_type=F32)
        total = part if total is None else total + part
    out_ref[...] = total.astype(out_ref.dtype)


def expert_body(n_in, *refs):
    ins, (gates, ups, downs), refs = refs[:n_in], refs[n_in : n_in + 3], refs[n_in + 3 :]
    outs, (rows, hidden) = refs[:n_in], refs[n_in:]
    at = 0
    for ref in ins:
        rows[at : at + ref.shape[0]] = ref[...]
        at += ref.shape[0]

    def into(j, carry):
        columns = pl.ds(pl.multiple_of(j * LANES, LANES), LANES)
        both = jnp.concatenate([gates[:, columns], ups[:, columns]], axis=1)
        both = jnp.dot(rows[...], both, preferred_element_type=F32)
        gate_out, up_out = both[:, :LANES], both[:, LANES:]
        hidden[:, columns] = (gate_out * jax.nn.sigmoid(gate_out) * up_out).astype(BF16)
        return carry

    lax.fori_loop(0, gates.shape[1] // LANES, into, 0)

    def out_of(j, carry):
        columns = pl.ds(pl.multiple_of(2 * j * LANES, 2 * LANES), 2 * LANES)
        result = jnp.dot(hidden[...], downs[:, columns], preferred_element_type=F32).astype(BF16)
        at = 0
        for out in outs:
            out[:, columns] = result[at : at + out.shape[0]]
            at += out.shape[0]
        return carry

    lax.fori_loop(0, downs.shape[1] // (2 * LANES), out_of, 0)


def all_rows(block, way):
    if way:
        from_left = moved(block, "x", 1)
        from_right = moved(block, "x", -1)
        far = moved(from_left if way > 0 else from_right, "x", way)
        return (block, from_left, from_right), (far,)
    half = block.shape[0] // 2
    own_a, own_b = block[:half], block[half:]
    left_a = moved(own_a, "x", 1)
    right_b = moved(own_b, "x", -1)
    left_b = moved(own_b, "x", 1)
    right_a = moved(own_a, "x", -1)
    far = moved(left_a, "x", 1), moved(right_b, "x", -1)
    return (own_a, own_b, left_a, left_b, right_a, right_b), far


def expert_parts(rows, weights):
    count, wide = sum(x.shape[0] for x in rows), rows[0].shape[1]
    part = weights[0].shape[1]
    run = call(
        functools.partial(expert_body, len(rows)),
        [shape(x.shape) for x in rows],
        [VMEM] * (len(rows) + 3),
        scratch=[pltpu.VMEM((count, wide), BF16), pltpu.VMEM((count, part), BF16)],
        flops=count * 2 * wide * 3 * part,
        limit=EXPERT_LIMIT,
    )
    return run(*rows, *weights)


def added(*terms):
    return functools.reduce(jnp.add, [term.astype(F32) for term in terms]).astype(BF16)


def summed(near, away, way):
    if way:
        own, left, right = near
        relay = moved(away[0], "x", way)
        left, right = (left, added(right, relay)) if way > 0 else (added(left, relay), right)
        low = moved(right, "x", 1)
        high = moved(left, "x", -1)
        return added(own, low, high)
    own_a, own_b, left_a, left_b, right_a, right_b = near
    low_b = moved(right_b, "x", 1)
    high_a = moved(left_a, "x", -1)
    relay_a = moved(away[0], "x", 1)
    relay_b = moved(away[1], "x", -1)
    low_a = moved(added(right_a, relay_a), "x", 1)
    high_b = moved(added(left_b, relay_b), "x", -1)
    return jnp.concatenate([added(own_a, low_a, high_a), added(own_b, low_b, high_b)])


def exchanged(rows, devices):
    wide = rows.shape[1]
    flat = rows.reshape(devices, -1, 128)
    flat = lax.all_to_all(flat, YC, 0, 0, tiled=True)
    return flat.reshape(-1, wide)


def step(
    cell_query_rows,
    cell_key_rows,
    cell_value_rows,
    output_gate_logits,
    log_input_gate,
    forget_gate_logits,
    extra_log_forget,
    cell_output_scale,
    tokens_into_experts,
    expert_norm_scale,
    token_expert_index,
    chosen_expert_weight,
    expert_gate_weight,
    expert_up_weight,
    expert_down_weight,
):
    where = jnp.stack([lax.axis_index(name) for name in ALL]).astype(jnp.int32)
    gates = (log_input_gate, forget_gate_logits, extra_log_forget)
    experts = lax.axis_size(YC)
    n_tok, wide = tokens_into_experts.shape
    weights = (expert_gate_weight[0], expert_up_weight[0], expert_down_weight[0])
    blocks = call(
        functools.partial(dispatch_body, experts, GROUPS),
        [shape((experts * (high - low), wide)) for low, high in GROUPS],
        [pl.BlockSpec(memory_space=pltpu.HBM)] * 2 + [VMEM],
        scratch=[
            pltpu.VMEM((n_tok, wide), BF16),
            pltpu.VMEM((1, wide), F32),
            pltpu.SemaphoreType.DMA((2,)),
        ],
        flops=1 << 28,
    )(
        pltpu.with_memory_space_constraint(tokens_into_experts, pltpu.HBM),
        pltpu.with_memory_space_constraint(expert_norm_scale.reshape(1, -1), pltpu.HBM),
        token_expert_index.T,
    )

    def gathered(at, result, *total):
        low, high = GROUPS[at]
        last = at == len(GROUPS) - 1
        return call(
            functools.partial(gather_body, experts, low, high),
            shape((n_tok, wide), BF16 if last else F32),
            [VMEM] * (3 + len(total)),
            flops=1 << 28,
        )(token_expert_index.T, chosen_expert_weight.T, result, *total)

    packed, packed_wide = shape(PACKED), shape(PACKED, F32)
    first = exchanged(blocks[0], experts)
    own, other = call(totals_body, [packed] * 2, [SMEM] + [VMEM] * 5, flops=1 << 27)(
        where, cell_key_rows, cell_value_rows, *gates
    )
    other = flipped(other, "c", 0)
    sent, whole = call(chip_body, [packed, packed_wide], [SMEM] + [VMEM] * 2, flops=1 << 25)(where, own, other)
    before = ()
    bits = [(axis, bit) for axis in "yz" for bit in range(lax.axis_size(axis).bit_length() - 1)]
    for axis, bit in bits[:-1]:
        got = flipped(sent, axis, bit)
        sent, whole, *before = call(
            functools.partial(double_body, ALL.index(axis), bit),
            [packed, packed_wide, packed_wide],
            [SMEM] + [VMEM] * (2 + len(before)),
            flops=JOIN_FLOPS,
        )(where, got, whole, *before)
    axis, bit = bits[-1]
    got = flipped(sent, axis, bit)
    mine, partner = call(
        functools.partial(prefix_body, ALL.index(axis), bit), [packed] * 2, [SMEM] + [VMEM] * 4, flops=1 << 26
    )(where, got, *before, own, other)
    arrived = flipped(partner, "c", 0)
    mixed = call(outputs_body, shape(cell_query_rows.shape), [SMEM] + [VMEM] * 10, flops=1 << 28)(
        where,
        cell_query_rows,
        cell_key_rows,
        cell_value_rows,
        output_gate_logits,
        *gates,
        cell_output_scale.reshape(1, -1),
        mine,
        arrived,
    )
    total = ()
    for at, way in enumerate(WAYS):
        block = first if at == 0 else exchanged(blocks[at], experts)
        near, far = all_rows(block, way)
        near, far = expert_parts(near, weights), expert_parts(far, weights)
        result = exchanged(summed(near, far, way), experts)
        total = (gathered(at, result, *total),)
    expert_output = total[0]
    return (mixed, expert_output)


def solution(mesh):
    devices = mesh.devices
    finer = Mesh(devices.reshape(-1, 4, 2, mesh.shape["tp"]), ALL)
    placed = (
        P(YC, "x"),
        P(YC, "x"),
        P(YC, "x"),
        P(YC, "x"),
        P("x", YC),
        P("x", YC),
        P("x", YC),
        P("x"),
        P(ALL, None),
        P(),
        P(ALL, None),
        P(ALL, None),
        P(YC, None, "x"),
        P(YC, None, "x"),
        P(YC, "x", None),
    )
    return jax.shard_map(step, mesh=finer, in_specs=placed, out_specs=(P(YC, "x"), P(ALL, None)), check_vma=False)
```
